256 devices in a mesh: grp: 2 (over z), sp: 16 (over y, core), tp: 8 (over x).
Axes of the slice: x: 8, y: 8, z: 2, core: 2. Of those that a mesh axis runs over, the one named last changes fastest.
The devices are a block of a 8x8x16 slice.
Arguments:
- resid_in: bfloat16 [32768, 2048], P(('grp', 'sp', 'tp')), parts along dimension 0, may hold values from -6 to 6
- pool_input: bfloat16 [32768, 1024], P(('grp', 'sp'), 'tp'), parts along dimension 0, may hold values from -6 to 6
- pool_weight: bfloat16 [4, 256, 256], replicated, may hold values from -0.375 to 0.375
- pool_scale: float32 [1024], replicated, may hold values from 0.2 to 0.8
- out_weight: bfloat16 [1024, 2048], replicated, may hold values from -0.1875 to 0.1875
- mix_gain: float32 [2048], replicated, may hold values from 0.1 to 1.9
- ffn_gain: float32 [2048], replicated, may hold values from 0.1 to 1.9
- w_gate: bfloat16 [32, 2048, 1024], P('sp', None, 'tp'), may hold values from -0.375 to 0.375
- w_up: bfloat16 [32, 2048, 1024], P('sp', None, 'tp'), may hold values from -0.375 to 0.375
- w_down: bfloat16 [32, 1024, 2048], P('sp', 'tp'), may hold values from -0.1875 to 0.1875
- routes: int32 [32768, 2], P(('grp', 'sp', 'tp')), parts along dimension 0, may hold values from 0 to 31, all different within a row; in each aligned block of 128 rows (0 to 127, 128 to 255, ...) at most 9 rows name the same one
- route_weight: float32 [32768, 2], P(('grp', 'sp', 'tp')), parts along dimension 0, may hold values from 0.1 to 1
- post_gain: float32 [2048], replicated, may hold values from 0.1 to 1.9
Outputs:
- layer_out: bfloat16 [32768, 2048], P(('grp', 'sp', 'tp')), parts along dimension 0
The draws below stay inside these ranges and needn't reach their ends.
There are 2 independent parts, one for each index of `grp`. The reference program is written for one: setup_inputs(seed, part) draws one part's arguments, and reference() takes and returns one part's arrays. A program takes and returns all parts, laid end to end along the dimension named above; an argument that names none is the same for every part. Nothing has to cross between parts.
Inputs may be any that keep to these rules, and one draw needn't show every extreme that they name: `routes`: each row names 2 different experts. The rows of one device name any one expert at most 9 times, and in every draw some device's rows name some expert exactly 9 times.
All inputs are finite; a program needn't handle non-finite values.
Results may differ from the reference program's by a relative error of at most 0.011.
Values may be sent and summed in bfloat16 or wider, within the bound.
A program may use at most 128 MiB of HBM per device.

```python
import math
import jax
import jax.numpy as jnp
import numpy as np
from jax import lax

D = 2048
POOL_WIDTH = 1024
GROUPS = 4
GROUP_DIM = 256
FF = 1024
EXPERTS = 32
TOP = 2
TOK_DEV = 128
CAP = 9
SEQ = 16384
N_TP = 8


def shard_levels(key, shape, cuts, smallest, high):
    gain, own = 1.0, jax.random.fold_in(key, 6)
    for axis_at, shards_of in cuts:
        draws = jnp.exp(jax.random.uniform(jax.random.fold_in(own, axis_at), (shards_of,), jnp.float32, smallest / len(cuts), high / len(cuts)))
        gain = gain * jnp.repeat(draws, shape[axis_at] // shards_of).reshape([-1 if axis == axis_at else 1 for axis in range(len(shape))])
    return gain


def assign_block(own_key, own, number, rows, number_of, top, bound, skew):
    order = jax.random.permutation(own_key, number_of)
    packed, ordinary = shares(number_of, rows * top, bound, skew, True), shares(number_of, rows * top, bound, skew, False)
    places = jnp.arange(number_of)

    def named(sizes, offset_by):
        used = int((sizes > 0).sum())
        fixed = max(1, used // 4)
        passed = fixed + (places - fixed + offset_by * (used - fixed)) % max(1, number_of - fixed)
        return jnp.zeros((number_of,), jnp.int32).at[order[jnp.where(places < fixed, places, passed)]].set(jnp.asarray(sizes, jnp.int32))

    sizes = jnp.where(number % 4 == 0, named(packed, number // 4), named(ordinary, number - number // 4 - 1))
    mixed = jax.random.permutation(jax.random.fold_in(own, 3), number_of)
    source_of, sink = mixed[0:number_of // 2 * 2:2], mixed[1:number_of // 2 * 2:2]
    margin = jnp.minimum(sizes[source_of] - 1, bound - sizes[sink]) // 2
    margin = jnp.where((source_of == order[0]) | (sink == order[0]) | (sizes[sink] == 0), 0, jnp.maximum(margin, 0))
    passed = jax.random.randint(jax.random.fold_in(own, 4), (number_of // 2,), 0, 1 << 20) % (margin + 1)
    sizes = sizes.at[source_of].add(-passed).at[sink].add(passed)
    labels = jnp.searchsorted(jnp.cumsum(sizes), jnp.arange(rows * top), side="right").astype(jnp.int32)
    listing = labels.reshape(top, rows).T
    listing = listing[jax.random.permutation(jax.random.fold_in(own, 1), rows)]
    offset_by = jax.random.randint(jax.random.fold_in(own, 2), (rows, 1), 0, top)
    return jnp.take_along_axis(listing, (jnp.arange(top)[None, :] + offset_by) % top, axis=1)


def shares(count, total, limit, slope, full):
    portions = [(1 << 20) // math.isqrt(standing ** slope) + 1 for standing in range(1, count + 1)]
    largest = limit if full else min(limit, max(-(-total // count), total * portions[0] // sum(portions)))
    least = 1 if total - largest >= count - 1 else 0
    given, surplus = [largest] + [least] * (count - 1), total - largest - least * (count - 1)
    while surplus > 0:
        candidates = [i for i in range(1, count) if given[i] < largest] or [i for i in range(1, count) if given[i] < limit]
        pool, budget = sum([portions[i] for i in candidates]), surplus
        for i in candidates:
            more = min(limit - given[i], max(1, budget * portions[i] // pool), surplus)
            given[i] = given[i] + more
            surplus = surplus - more
    return np.array(given)


def gaussian(stream_key, extent, width, limit, split=(), kind=jnp.bfloat16):
    gain = shard_levels(stream_key, extent, split, -0.22, 0.18) if split else 1.0
    array = jax.random.normal(stream_key, extent, jnp.float32) * width * gain
    return jnp.minimum(jnp.maximum(array, -limit), limit).astype(kind)


def setup_inputs(seed: int = 0, part: int = 0) -> dict:
    seeds = jax.random.split(jax.random.key(seed), 14)
    own_keys = jax.random.split(jax.random.fold_in(seeds[13], part), 14)
    resid_in = gaussian(own_keys[0], (SEQ, D), 1.0, 6.0, ((0, 128),))
    pool_input = gaussian(own_keys[1], (SEQ, POOL_WIDTH), 1.0, 6.0, ((0, 16), (1, 8)))
    pool_weight = gaussian(seeds[2], (GROUPS, GROUP_DIM, GROUP_DIM), GROUP_DIM ** -0.5, 0.375)
    pool_scale = jnp.clip(jax.random.uniform(seeds[3], (POOL_WIDTH,), jnp.float32, 0.2, 0.8), 0.2, 0.8)
    out_weight = gaussian(seeds[4], (POOL_WIDTH, D), POOL_WIDTH ** -0.5, 0.1875)
    mix_gain = jnp.clip(1.0 + 0.18 * jax.random.normal(seeds[5], (D,), jnp.float32), 0.1, 1.9)
    ffn_gain = jnp.clip(1.0 + 0.18 * jax.random.normal(seeds[6], (D,), jnp.float32), 0.1, 1.9)
    w_gate = gaussian(seeds[7], (EXPERTS, D, FF), (D // 8) ** -0.5, 0.375, ((0, 16), (2, 8)))
    w_up = gaussian(seeds[8], (EXPERTS, D, FF), (D // 8) ** -0.5, 0.375, ((0, 16), (2, 8)))
    w_down = gaussian(seeds[9], (EXPERTS, FF, D), FF ** -0.5, 0.1875, ((0, 16), (1, 8)))
    routes_keys = jax.random.split(jax.random.fold_in(own_keys[10], 1), SEQ // TOK_DEV)
    routes_turns = jax.random.permutation(jax.random.fold_in(own_keys[10], 3), SEQ // TOK_DEV)
    routes = jax.vmap(lambda own, number: assign_block(jax.random.fold_in(own_keys[10], 2), own, number, TOK_DEV, EXPERTS, TOP, CAP, 1))(routes_keys, routes_turns).reshape((SEQ, TOP))
    route_weight = jnp.clip(jnp.exp(math.log(1.0) - 2.3025851 * jax.random.uniform(own_keys[11], (SEQ, TOP), jnp.float32) ** shard_levels(own_keys[11], (SEQ, TOP), ((0, 128),), -0.2, 0.2)), 0.1, 1.0)
    post_gain = jnp.clip(1.0 + 0.18 * jax.random.normal(seeds[12], (D,), jnp.float32), 0.1, 1.9)
    return {"resid_in": resid_in, "pool_input": pool_input, "pool_weight": pool_weight, "pool_scale": pool_scale, "out_weight": out_weight, "mix_gain": mix_gain, "ffn_gain": ffn_gain, "w_gate": w_gate, "w_up": w_up, "w_down": w_down, "routes": routes, "route_weight": route_weight, "post_gain": post_gain}


pool_windows = (2, 4, 8, 16)
reach_back = 15
norm_eps = 1e-06
clamp_limit = 7.0
glu_alpha = 1.702

def rms_scale(values, gain_vec):
    inverse = lax.rsqrt(lax.optimization_barrier(jnp.mean(values * values, axis=-1, keepdims=True)) + norm_eps)
    return values * inverse * gain_vec

def clamped_unit(gate_pre, upward):
    gate_clip = jnp.minimum(gate_pre, clamp_limit)
    linear = jnp.clip(upward, -clamp_limit, clamp_limit)
    return gate_clip * jax.nn.sigmoid(glu_alpha * gate_clip) * (linear + 1.0)

def reference(resid_in, pool_input, pool_weight, pool_scale, out_weight, mix_gain, ffn_gain, w_gate, w_up, w_down, routes, route_weight, post_gain):
    source = pool_input.astype(jnp.float32)
    positions = jnp.arange(SEQ, dtype=jnp.int32)
    pieces = []
    for group_level, win_len in enumerate(pool_windows):
        group_cols = source[:, group_level * GROUP_DIM:(group_level + 1) * GROUP_DIM]
        padded = jnp.concatenate([jnp.zeros((reach_back, GROUP_DIM), jnp.float32), group_cols], axis=0)
        running = jnp.zeros((SEQ, GROUP_DIM), jnp.float32)
        for offset in range(win_len):
            running = running + padded[reach_back - offset:reach_back - offset + SEQ]
        divisor = jnp.minimum(positions + 1, win_len).astype(jnp.float32)[:, None]
        pieces.append(running / divisor - group_cols)
    mixed_rows = jnp.concatenate(pieces, axis=1).astype(jnp.bfloat16)
    pooled = jnp.einsum('tgc,gcd->tgd', mixed_rows.reshape(SEQ, GROUPS, GROUP_DIM).astype(jnp.float32), pool_weight.astype(jnp.float32))
    pooled = (pooled * pool_scale.reshape(GROUPS, GROUP_DIM)).astype(jnp.bfloat16).reshape(SEQ, POOL_WIDTH)
    mix_out = jnp.dot(pooled, out_weight, preferred_element_type=jnp.float32)
    residual = (resid_in.astype(jnp.float32) + rms_scale(mix_out, mix_gain)).astype(jnp.bfloat16)
    normed = rms_scale(residual.astype(jnp.float32), ffn_gain).astype(jnp.bfloat16)
    flat_route = routes.reshape(-1).astype(jnp.int32)
    total = SEQ * TOP
    sort_order = jnp.argsort(flat_route, stable=True).astype(jnp.int32)
    token_of = (sort_order // TOP).astype(jnp.int32)
    counts = lax.optimization_barrier(jnp.sum((flat_route[:, None] == jnp.arange(EXPERTS, dtype=jnp.int32)[None, :]).astype(jnp.int32), axis=0))
    starts = (jnp.cumsum(counts) - counts).astype(jnp.int32)
    most_rows = SEQ // TOK_DEV * CAP
    block_ff = FF // N_TP

    def one_expert(expert):
        row_index = jnp.minimum(starts[expert] + jnp.arange(most_rows, dtype=jnp.int32), total - 1)
        taken_rows = normed[token_of[row_index]]
        gate_pre = jnp.dot(taken_rows, w_gate[expert], preferred_element_type=jnp.float32)
        upward = jnp.dot(taken_rows, w_up[expert], preferred_element_type=jnp.float32)
        activated = clamped_unit(gate_pre, upward).astype(jnp.bfloat16)
        partials = jnp.einsum('rnf,nfd->rnd', activated.reshape(most_rows, N_TP, block_ff).astype(jnp.float32), w_down[expert].reshape(N_TP, block_ff, D).astype(jnp.float32))
        partials = lax.optimization_barrier(partials.astype(jnp.bfloat16))
        return lax.optimization_barrier(jnp.sum(partials.astype(jnp.float32), axis=1)).astype(jnp.bfloat16)
    expert_outs = lax.map(one_expert, jnp.arange(EXPERTS, dtype=jnp.int32))
    sorted_e = flat_route[sort_order]
    local_pos = (jnp.arange(total, dtype=jnp.int32) - starts[sorted_e]).astype(jnp.int32)
    picked = expert_outs[sorted_e, local_pos]
    assigned = jnp.zeros((total, D), jnp.bfloat16).at[sort_order].set(picked)
    expert_mix = lax.optimization_barrier(jnp.sum(assigned.reshape(SEQ, TOP, D).astype(jnp.float32) * route_weight[:, :, None], axis=1))
    return (residual.astype(jnp.float32) + rms_scale(expert_mix, post_gain)).astype(jnp.bfloat16)
```

```python
import functools

import jax
import jax.numpy as jnp
from jax import lax
from jax.experimental import pallas as pl
from jax.experimental.pallas import tpu as pltpu
from jax.sharding import PartitionSpec as P

GROUPS = 4
GROUP_DIM = 256
TOP = 2
CAP = 9
MAIN = 8
CORES = 2

pool_windows = (2, 4, 8, 16)
halo_rows = 16
norm_eps = 1e-06
clamp_limit = 7.0
glu_alpha = 1.702
MESH = pl.DeviceIdType.MESH
F32 = jnp.float32
BF16 = jnp.bfloat16


def dot(a, b):
    return jnp.dot(a, b, preferred_element_type=F32)


def rows_of(block):
    wide = block.astype(F32)
    return wide.reshape(-1, wide.shape[-1]).astype(BF16)


def kernel(
    n_sp, n_tp,
    pin, resid, pool_w, pool_s, out_w, mix_g, ffn_g, w_gate, w_up, w_down, routes, route_w, post_g,
    out,
    ext, mixbuf, tokmix, pool_wv, out_wv, pooled, wide, resbuf, normbuf, whi, wlo,
    disp, yarr, ovout, wgu, wd, rows, xb, act, orow, ret, ovback, fin, outbuf,
    lsem, halo_s, halo_r, pool_sem_s, pool_sem_r, w_s, w_r, f_s, f_r,
    y_s, y_r, x_s, x_r, o_s, o_r, b_s, b_r, v_s, v_r,
):
    n_y = n_sp // CORES
    local_experts = w_gate.shape[0]
    row_experts = local_experts * CORES
    blocks = row_experts + 1
    slots_row = blocks * 8
    step = n_tp // row_experts
    seg, channels = pin.shape
    tok, width = resid.shape
    ff = w_gate.shape[2]
    sp = lax.axis_index("sp")
    tp = lax.axis_index("tp")
    y = sp // CORES
    core = sp % CORES
    par = y % step
    mine = tp // step
    active = tp % step == par
    mate = y * CORES + (1 - core)

    def home(j):
        return j * step + par

    def at_y(row):
        return row * CORES + core

    def remote(src, dst, send, recv, **where):
        return pltpu.make_async_remote_copy(
            src_ref=src, dst_ref=dst, send_sem=send, recv_sem=recv, device_id=where, device_id_type=MESH
        )

    def landed(dst, sem):
        pltpu.make_async_copy(dst, dst, sem).wait()

    loads = [
        pltpu.make_async_copy(pin, ext.at[pl.ds(halo_rows, seg)], lsem.at[0]),
        pltpu.make_async_copy(pool_w, pool_wv, lsem.at[1]),
        pltpu.make_async_copy(out_w, out_wv, lsem.at[2]),
        pltpu.make_async_copy(resid, resbuf, lsem.at[3]),
    ]
    for load in loads:
        load.start()

    barrier = pltpu.get_barrier_semaphore()
    for d in range(1, n_tp):
        pl.semaphore_signal(barrier, inc=1, device_id={"tp": (tp + d) % n_tp}, device_id_type=MESH)
    for d in range(1, n_y):
        pl.semaphore_signal(barrier, inc=1, device_id={"sp": at_y((y + d) % n_y)}, device_id_type=MESH)
    beside = (sp + 2 * core - 1 + n_sp) % n_sp
    pl.semaphore_signal(barrier, inc=1, device_id={"sp": mate}, device_id_type=MESH)
    pl.semaphore_signal(barrier, inc=1, device_id={"sp": beside}, device_id_type=MESH)
    pl.semaphore_wait(barrier, n_tp + n_y)

    halo = remote(
        pin.at[pl.ds(seg - halo_rows, halo_rows)], ext.at[pl.ds(0, halo_rows)], halo_s, halo_r, sp=(sp + 1) % n_sp
    )
    halo.start()
    loads[0].wait()
    halo.wait()
    at = lax.broadcasted_iota(jnp.int32, (halo_rows + seg, 1), 0)
    own = ext[...].astype(F32)
    own = jnp.where(jnp.logical_and(at < halo_rows, sp == 0), 0.0, own)
    group = tp * channels // GROUP_DIM
    total, picked = own, own
    for level, window in enumerate(pool_windows):
        total = total + pltpu.roll(total, window // 2, 0)
        picked = jnp.where(group == level, total, picked)
    window = lax.shift_left(jnp.int32(2), group.astype(jnp.int32))
    divisor = jnp.minimum(sp * seg + at - halo_rows + 1, window).astype(F32)
    mixed = picked / jnp.maximum(divisor, 1.0) - own
    mixbuf[...] = mixed[halo_rows:].astype(BF16)

    def pool_copy(d):
        to = (tp + d) % n_tp
        return remote(
            mixbuf.at[pl.ds(to * tok, tok)], tokmix.at[tp], pool_sem_s.at[d], pool_sem_r.at[d], tp=to
        )

    keep = pltpu.make_async_copy(mixbuf.at[pl.ds(tp * tok, tok)], tokmix.at[tp], pool_sem_r.at[0])
    keep.start()
    for d in range(1, n_tp):
        pool_copy(d).start()

    def weight_copies(e):
        col = home(core * local_experts + e)
        half = [pl.ds(0, ff), pl.ds(ff, ff)]
        pairs = [
            (w_gate.at[e], wgu.at[tp, :, half[0]]),
            (w_up.at[e], wgu.at[tp, :, half[1]]),
            (w_down.at[e], wd.at[pl.ds(tp * ff, ff)]),
        ]
        far = lambda: [remote(s, t, w_s.at[e, i], w_r.at[i, tp], tp=col) for i, (s, t) in enumerate(pairs)]
        near = lambda: [pltpu.make_async_copy(s, t, w_r.at[i, tp]) for i, (s, t) in enumerate(pairs)]
        return col, far, near

    for e in range(local_experts):
        col, far, near = weight_copies(e)

        @pl.when(col != tp)
        def _():
            for copy in far():
                copy.start()

        @pl.when(col == tp)
        def _():
            for copy in near():
                copy.start()

    lanes = whi.shape[1]
    expert_lane = lax.broadcasted_iota(jnp.int32, (tok, 128), 1)
    before = (
        lax.broadcasted_iota(jnp.int32, (tok, tok), 1) < lax.broadcasted_iota(jnp.int32, (tok, tok), 0)
    ).astype(F32).astype(BF16)
    named = [routes[:, k : k + 1] for k in range(TOP)]
    onehot = [(named[k] == expert_lane).astype(F32) for k in range(TOP)]
    earlier = jnp.zeros((1, 128), F32)
    slot_lane = lax.broadcasted_iota(jnp.int32, (1, lanes), 1)
    inside = slot_lane % slots_row
    spill = inside >= row_experts * MAIN
    row_expert = jnp.where(spill, inside - row_experts * MAIN, inside // MAIN)
    slot_rank = jnp.where(spill, MAIN, inside % MAIN).astype(F32)
    valid = jnp.logical_and(row_expert < row_experts, slot_lane < n_y * slots_row)
    slot_expert = jnp.where(valid, slot_lane // slots_row * row_experts + row_expert, -1)
    pick = jnp.zeros((tok, lanes), F32)
    comb = jnp.zeros((tok, lanes), F32)
    for k in range(TOP):
        ranks = dot(before, onehot[k].astype(BF16)) + earlier
        rank = jnp.sum(ranks * onehot[k], axis=1, keepdims=True)
        earlier = earlier + jnp.sum(onehot[k], axis=0, keepdims=True)
        hit = jnp.logical_and(named[k] == slot_expert, rank == slot_rank).astype(F32)
        pick = pick + hit
        comb = comb + hit * route_w[:, k : k + 1]
    high = comb.astype(BF16)
    whi[...] = high
    wlo[...] = (comb - high.astype(F32)).astype(BF16)
    pick_rows = jnp.transpose(pick)[: n_y * slots_row].astype(BF16)

    keep.wait()
    for d in range(1, n_tp):
        pool_copy(d).wait()
    loads[1].wait()
    per = GROUP_DIM // channels
    for g in range(GROUPS):
        mixed_g = jnp.concatenate([tokmix[g * per + i] for i in range(per)], axis=1)
        cols = slice(g * GROUP_DIM, (g + 1) * GROUP_DIM)
        pooled[:, cols] = (dot(mixed_g, pool_wv[g]) * pool_s[:, cols]).astype(BF16)
    loads[2].wait()
    tile = 256

    @pl.loop(0, width // tile)
    def _(n):
        cols = pl.ds(pl.multiple_of(n * tile, tile), tile)
        wide[:, cols] = dot(pooled[...], out_wv[:, cols])

    loads[3].wait()
    part = 32

    def scaled(values, gain):
        inverse = lax.rsqrt(jnp.mean(values * values, axis=-1, keepdims=True) + norm_eps)
        return values * inverse * gain[...]

    @pl.loop(0, tok // part)
    def _(r):
        at = pl.ds(pl.multiple_of(r * part, part), part)
        residual = (resbuf[at, :].astype(F32) + scaled(wide[at, :], mix_g)).astype(BF16)
        resbuf[at, :] = residual
        normbuf[at, :] = scaled(residual.astype(F32), ffn_g).astype(BF16)

    @pl.loop(0, width // tile)
    def _(n):
        cols = pl.ds(pl.multiple_of(n * tile, tile), tile)
        sent = dot(pick_rows, normbuf[:, cols])
        disp[:, :, :, cols] = sent.reshape(n_y, blocks, 8, tile).astype(BF16)

    def y_copy(d):
        to = (y + d) % n_y
        return remote(disp.at[to], yarr.at[y], y_s.at[d], y_r.at[d], sp=at_y(to))

    y_keep = pltpu.make_async_copy(disp.at[y], yarr.at[y], y_r.at[0])
    y_keep.start()
    for d in range(1, n_y):
        y_copy(d).start()
    y_keep.wait()
    for d in range(1, n_y):
        y_copy(d).wait()

    count = n_y * 8
    to_row = lax.broadcasted_iota(jnp.int32, (row_experts * n_y, count), 0)
    from_row = lax.broadcasted_iota(jnp.int32, (row_experts * n_y, count), 1)
    regroup = (from_row == to_row % n_y * 8 + to_row // n_y).astype(F32).astype(BF16)

    @pl.loop(0, width // tile)
    def _(n):
        cols = pl.ds(pl.multiple_of(n * tile, tile), tile)
        moved = dot(regroup, rows_of(yarr[:, row_experts, :, cols]))
        ovout[:, :, cols] = moved.reshape(row_experts, n_y, tile).astype(BF16)

    def x_copies(k):
        j = (mine + 1 + k) % row_experts
        col = home(j)
        pairs = [(yarr.at[:, j], rows.at[tp, pl.ds(0, n_y)]), (ovout.at[j], rows.at[tp, n_y])]
        far = lambda: [remote(s, t, x_s.at[k, i], x_r.at[i, tp], tp=col) for i, (s, t) in enumerate(pairs)]
        near = lambda: [pltpu.make_async_copy(s, t, x_r.at[i, tp]) for i, (s, t) in enumerate(pairs)]
        return col, far, near

    for k in range(row_experts):
        col, far, near = x_copies(k)

        @pl.when(col != tp)
        def _():
            for copy in far():
                copy.start()

        @pl.when(col == tp)
        def _():
            for copy in near():
                copy.start()

    owner = mine // local_experts == core

    def forward_copies(s):
        shard = pl.ds(s * ff, ff)
        return [
            remote(wgu.at[s], wgu.at[s], f_s.at[0, s], f_r.at[0, s], sp=mate),
            remote(wd.at[shard], wd.at[shard], f_s.at[1, s], f_r.at[1, s], sp=mate),
        ]

    @pl.when(jnp.logical_and(active, owner))
    def _():
        for d in (0, 1, -1, 2, -2, 3, -3, 4):
            s = (tp + d + n_tp) % n_tp
            landed(wgu.at[s, :, pl.ds(0, ff)], w_r.at[0, s])
            landed(wgu.at[s, :, pl.ds(ff, ff)], w_r.at[1, s])
            landed(wd.at[pl.ds(s * ff, ff)], w_r.at[2, s])
            for copy in forward_copies(s):
                copy.start()

    @pl.when(jnp.logical_and(active, jnp.logical_not(owner)))
    def _():
        for s in range(n_tp):
            landed(wgu.at[s], f_r.at[0, s])
            landed(wd.at[pl.ds(s * ff, ff)], f_r.at[1, s])

    def out_copy(s):
        return remote(orow.at[s], ret.at[mine], o_s.at[s], o_r.at[mine], tp=s)

    pair = 2
    held = n_y + 1

    @pl.when(active)
    def _():
        @pl.loop(0, n_tp // pair)
        def _(q):
            first = (tp + q * pair) % n_tp
            sources = [(first + i) % n_tp for i in range(pair)]
            for i, s in enumerate(sources):
                landed(rows.at[s, pl.ds(0, n_y)], x_r.at[0, s])
                landed(rows.at[s, n_y], x_r.at[1, s])
                xb[pl.ds(i * 8 * held, 8 * held), :] = rows_of(rows[s])

            @pl.loop(0, n_tp)
            def _(s):
                both = dot(xb[...], wgu[s])
                gate = jnp.minimum(both[:, :ff], clamp_limit)
                linear = jnp.clip(both[:, ff:], -clamp_limit, clamp_limit)
                cols = pl.ds(pl.multiple_of(s * ff, ff), ff)
                act[:, cols] = (gate * jax.nn.sigmoid(glu_alpha * gate) * (linear + 1.0)).astype(BF16)

            @pl.loop(0, width // tile)
            def _(n):
                cols = pl.ds(pl.multiple_of(n * tile, tile), tile)
                result = dot(act[...], wd[:, cols])
                for i, s in enumerate(sources):
                    piece = result[i * 8 * held : (i + 1) * 8 * held]
                    orow[s, :, :, cols] = piece.reshape(held, 8, tile).astype(BF16)

            for s in sources:
                @pl.when(s != tp)
                def _():
                    out_copy(s).start()

                @pl.when(s == tp)
                def _():
                    pltpu.make_async_copy(orow.at[s], ret.at[mine], o_r.at[mine]).start()

    for k in range(row_experts):
        landed(ret.at[k], o_r.at[k])
    to_row = lax.broadcasted_iota(jnp.int32, (count, row_experts * n_y), 0)
    from_row = lax.broadcasted_iota(jnp.int32, (count, row_experts * n_y), 1)
    regroup_back = (from_row == to_row % 8 * n_y + to_row // 8).astype(F32)
    regroup_back = jnp.where(to_row % 8 < row_experts, regroup_back, 0.0).astype(BF16)

    def b_copies(d):
        to = (y + d) % n_y
        main = lambda: remote(ret.at[:, to], fin.at[y, pl.ds(0, row_experts)], b_s.at[d], b_r.at[d], sp=at_y(to))
        over = lambda: remote(ovback.at[to], fin.at[y, row_experts], v_s.at[d], v_r.at[d], sp=at_y(to))
        return main, over

    b_keep = pltpu.make_async_copy(ret.at[:, y], fin.at[y, pl.ds(0, row_experts)], b_r.at[0])
    b_keep.start()
    for d in range(1, n_y):
        b_copies(d)[0]().start()

    @pl.loop(0, width // tile)
    def _(n):
        cols = pl.ds(pl.multiple_of(n * tile, tile), tile)
        moved = dot(regroup_back, rows_of(ret[:, n_y, :, cols]))
        ovback[:, :, cols] = moved.reshape(n_y, 8, tile).astype(BF16)

    v_keep = pltpu.make_async_copy(ovback.at[y], fin.at[y, row_experts], v_r.at[0])
    v_keep.start()
    for d in range(1, n_y):
        b_copies(d)[1]().start()
    b_keep.wait()
    v_keep.wait()
    for d in range(1, n_y):
        for copy in b_copies(d):
            copy().wait()

    @pl.loop(0, width // tile)
    def _(n):
        cols = pl.ds(pl.multiple_of(n * tile, tile), tile)
        came = rows_of(fin[:, :, :, cols])
        came = jnp.concatenate([came, jnp.zeros((lanes - n_y * slots_row, tile), BF16)], axis=0)
        wide[:, cols] = dot(whi[...], came) + dot(wlo[...], came)

    @pl.loop(0, tok // part)
    def _(r):
        at = pl.ds(pl.multiple_of(r * part, part), part)
        outbuf[at, :] = (resbuf[at, :].astype(F32) + scaled(wide[at, :], post_g)).astype(BF16)

    result = pltpu.make_async_copy(outbuf, out, lsem.at[0])
    result.start()

    for e in range(local_experts):
        col, far, near = weight_copies(e)

        @pl.when(col != tp)
        def _():
            for copy in far():
                copy.wait_send()

    for k in range(row_experts):
        col, far, near = x_copies(k)

        @pl.when(col != tp)
        def _():
            for copy in far():
                copy.wait_send()

    @pl.when(jnp.logical_and(active, owner))
    def _():
        for s in range(n_tp):
            for copy in forward_copies(s):
                copy.wait_send()

    @pl.when(active)
    def _():
        for s in range(n_tp):
            @pl.when(s != tp)
            def _():
                out_copy(s).wait_send()

    result.wait()


def per_device(
    resid_in, pool_input, pool_weight, pool_scale, out_weight, mix_gain, ffn_gain,
    w_gate, w_up, w_down, routes, route_weight, post_gain,
):
    n_sp = lax.axis_size("sp")
    n_tp = lax.axis_size("tp")
    n_y = n_sp // CORES
    seg, channels = pool_input.shape
    tok, width = resid_in.shape
    local_experts, _, ff = w_gate.shape
    row_experts = local_experts * CORES
    blocks = row_experts + 1
    slots = n_y * blocks * 8
    lanes = -(-slots // 128) * 128
    held = n_y + 1
    dma = pltpu.SemaphoreType.DMA
    vmem = pltpu.VMEM
    whole = pl.BlockSpec(memory_space=pltpu.VMEM)
    there = pl.BlockSpec(memory_space=pl.ANY)
    scratch = [
        vmem((halo_rows + seg, channels), BF16),
        vmem((seg, channels), BF16),
        vmem((n_tp, tok, channels), BF16),
        vmem(pool_weight.shape, BF16),
        vmem(out_weight.shape, BF16),
        vmem((tok, pool_scale.shape[0]), BF16),
        vmem((tok, width), F32),
        vmem((tok, width), BF16),
        vmem((tok, width), BF16),
        vmem((tok, lanes), BF16),
        vmem((tok, lanes), BF16),
        vmem((n_y, blocks, 8, width), BF16),
        vmem((n_y, blocks, 8, width), BF16),
        vmem((row_experts, 8, width), BF16),
        vmem((n_tp, width, 2 * ff), BF16),
        vmem((n_tp * ff, width), BF16),
        vmem((n_tp, held, 8, width), BF16),
        vmem((2 * held * 8, width), BF16),
        vmem((2 * held * 8, n_tp * ff), BF16),
        vmem((n_tp, held, 8, width), BF16),
        vmem((row_experts, held, 8, width), BF16),
        vmem((n_y, 8, width), BF16),
        vmem((n_y, blocks, 8, width), BF16),
        vmem((tok, width), BF16),
        dma((4,)), dma, dma, dma((n_tp,)), dma((n_tp,)),
        dma((local_experts, 3)), dma((3, n_tp)), dma((2, n_tp)), dma((2, n_tp)),
        dma((n_y,)), dma((n_y,)), dma((row_experts, 2)), dma((2, n_tp)),
        dma((n_tp,)), dma((row_experts,)), dma((n_y,)), dma((n_y,)), dma((n_y,)), dma((n_y,)),
    ]
    return pl.pallas_call(
        functools.partial(kernel, n_sp, n_tp),
        out_shape=jax.ShapeDtypeStruct((tok, width), BF16),
        in_specs=[there, there, there, whole, there, whole, whole, there, there, there, whole, whole, whole],
        out_specs=there,
        scratch_shapes=scratch,
        compiler_params=pltpu.CompilerParams(
            collective_id=0, has_side_effects=True, vmem_limit_bytes=60 * 1024 * 1024
        ),
    )(
        pool_input, resid_in, pool_weight, pool_scale[None], out_weight, mix_gain[None], ffn_gain[None],
        w_gate, w_up, w_down, routes, route_weight, post_gain[None],
    )


def solution(mesh):
    in_specs = (
        P(("grp", "sp", "tp"), None),
        P(("grp", "sp"), "tp"),
        P(),
        P(),
        P(),
        P(),
        P(),
        P("sp", None, "tp"),
        P("sp", None, "tp"),
        P("sp", "tp", None),
        P(("grp", "sp", "tp"), None),
        P(("grp", "sp", "tp"), None),
        P(),
    )
    out_specs = P(("grp", "sp", "tp"), None)
    return jax.shard_map(
        per_device, mesh=mesh, in_specs=in_specs, out_specs=out_specs, check_vma=False
    )
```

```python
import functools

import jax
import jax.numpy as jnp
from jax import lax
from jax.experimental import pallas as pl
from jax.experimental.pallas import tpu as pltpu
from jax.sharding import PartitionSpec as P

GROUPS = 4
GROUP_DIM = 256
TOP = 2
CAP = 9
MAIN = 8
CORES = 2

pool_windows = (2, 4, 8, 16)
halo_rows = 16
norm_eps = 1e-06
clamp_limit = 7.0
glu_alpha = 1.702
MESH = pl.DeviceIdType.MESH
F32 = jnp.float32
BF16 = jnp.bfloat16


def dot(a, b):
    return jnp.dot(a, b, preferred_element_type=F32)


def rows_of(block):
    wide = block.astype(F32)
    return wide.reshape(-1, wide.shape[-1]).astype(BF16)


def kernel(
    n_sp, n_tp,
    pin, resid, pool_w, pool_s, out_w, mix_g, ffn_g, w_gate, w_up, w_down, routes, route_w, post_g,
    out,
    ext, mixbuf, tokmix, pool_wv, out_wv, pooled, wide, resbuf, normbuf, whi, wlo,
    disp, yarr, ovout, wgu, wd, rows, xb, act, kept, given, taken, orow, ret, ovback, fin, outbuf,
    lsem, halo_s, halo_r, pool_sem_s, pool_sem_r, w_s, w_r, f_s, f_r,
    y_s, y_r, x_s, x_r, n_s, n_r, p_s, p_r, o_s, o_r, b_s, b_r, v_s, v_r,
):
    n_y = n_sp // CORES
    local_experts = w_gate.shape[0]
    row_experts = local_experts * CORES
    step = n_tp // row_experts
    near = n_tp // step
    blocks = row_experts + 1
    slots_row = blocks * 8
    held = n_y + 1
    seg, channels = pin.shape
    tok, width = resid.shape
    ff = w_gate.shape[2]
    tile = 256
    part = 32
    scope = jax.named_scope
    sp = lax.axis_index("sp")
    tp = lax.axis_index("tp")
    y = sp // CORES
    core = sp % CORES
    mine = tp // step
    mate = y * CORES + (1 - core)
    side = tp % step
    sign = 2 * side - 1
    other = tp - sign

    def home(j):
        turn = (tp - step * j + 2 * n_tp - 1) % n_tp
        left = turn // near
        place = left * (near - 1 - turn % near) + (1 - left) * (turn % near)
        return step * j + 1 - left, place

    def source(d):
        return (tp + sign * d + n_tp) % n_tp

    def at_y(row):
        return row * CORES + core

    def remote(src, dst, send, recv, **where):
        return pltpu.make_async_remote_copy(
            src_ref=src, dst_ref=dst, send_sem=send, recv_sem=recv, device_id=where, device_id_type=MESH
        )

    def landed(dst, sem):
        pltpu.make_async_copy(dst, dst, sem).wait()

    def columns(n):
        return pl.ds(pl.multiple_of(n * tile, tile), tile)

    loads = [
        pltpu.make_async_copy(pin, ext.at[pl.ds(halo_rows, seg)], lsem.at[0]),
        pltpu.make_async_copy(pool_w, pool_wv, lsem.at[1]),
        pltpu.make_async_copy(out_w, out_wv, lsem.at[2]),
        pltpu.make_async_copy(resid, resbuf, lsem.at[3]),
    ]
    for load in loads:
        load.start()

    with scope("a_barrier"):
        barrier = pltpu.get_barrier_semaphore()
        for d in range(1, n_tp):
            pl.semaphore_signal(barrier, inc=1, device_id={"tp": (tp + d) % n_tp}, device_id_type=MESH)
        for d in range(1, n_y):
            pl.semaphore_signal(barrier, inc=1, device_id={"sp": at_y((y + d) % n_y)}, device_id_type=MESH)
        beside = (sp + 2 * core - 1 + n_sp) % n_sp
        pl.semaphore_signal(barrier, inc=1, device_id={"sp": mate}, device_id_type=MESH)
        pl.semaphore_signal(barrier, inc=1, device_id={"sp": beside}, device_id_type=MESH)
        pl.semaphore_wait(barrier, n_tp + n_y)

    with scope("b_mix"):
        halo = remote(
            pin.at[pl.ds(seg - halo_rows, halo_rows)], ext.at[pl.ds(0, halo_rows)], halo_s, halo_r, sp=(sp + 1) % n_sp
        )
        halo.start()
        loads[0].wait()
        halo.wait()
        at = lax.broadcasted_iota(jnp.int32, (halo_rows + seg, 1), 0)
        own = ext[...].astype(F32)
        own = jnp.where(jnp.logical_and(at < halo_rows, sp == 0), 0.0, own)
        group = tp * channels // GROUP_DIM
        total, picked = own, own
        for level, window in enumerate(pool_windows):
            total = total + pltpu.roll(total, window // 2, 0)
            picked = jnp.where(group == level, total, picked)
        window = lax.shift_left(jnp.int32(2), group.astype(jnp.int32))
        divisor = jnp.minimum(sp * seg + at - halo_rows + 1, window).astype(F32)
        mixed = picked / jnp.maximum(divisor, 1.0) - own
        mixbuf[...] = mixed[halo_rows:].astype(BF16)

    def pool_copy(d):
        to = (tp + d) % n_tp
        return remote(
            mixbuf.at[pl.ds(to * tok, tok)], tokmix.at[tp], pool_sem_s.at[d], pool_sem_r.at[d], tp=to
        )

    keep = pltpu.make_async_copy(mixbuf.at[pl.ds(tp * tok, tok)], tokmix.at[tp], pool_sem_r.at[0])
    keep.start()
    for d in range(1, n_tp):
        pool_copy(d).start()

    with scope("d_route"):
        lanes = whi.shape[1]
        expert_lane = lax.broadcasted_iota(jnp.int32, (tok, 128), 1)
        before = (
            lax.broadcasted_iota(jnp.int32, (tok, tok), 1) < lax.broadcasted_iota(jnp.int32, (tok, tok), 0)
        ).astype(F32).astype(BF16)
        named = [routes[:, k : k + 1] for k in range(TOP)]
        onehot = [(named[k] == expert_lane).astype(F32) for k in range(TOP)]
        earlier = jnp.zeros((1, 128), F32)
        slot_lane = lax.broadcasted_iota(jnp.int32, (1, lanes), 1)
        inside = slot_lane % slots_row
        spill = inside >= row_experts * MAIN
        row_expert = jnp.where(spill, inside - row_experts * MAIN, inside // MAIN)
        slot_rank = jnp.where(spill, MAIN, inside % MAIN).astype(F32)
        valid = jnp.logical_and(row_expert < row_experts, slot_lane < n_y * slots_row)
        slot_expert = jnp.where(valid, slot_lane // slots_row * row_experts + row_expert, -1)
        pick = jnp.zeros((tok, lanes), F32)
        comb = jnp.zeros((tok, lanes), F32)
        for k in range(TOP):
            ranks = dot(before, onehot[k].astype(BF16)) + earlier
            rank = jnp.sum(ranks * onehot[k], axis=1, keepdims=True)
            earlier = earlier + jnp.sum(onehot[k], axis=0, keepdims=True)
            hit = jnp.logical_and(named[k] == slot_expert, rank == slot_rank).astype(F32)
            pick = pick + hit
            comb = comb + hit * route_w[:, k : k + 1]
        high = comb.astype(BF16)
        whi[...] = high
        wlo[...] = (comb - high.astype(F32)).astype(BF16)
        pick_rows = jnp.transpose(pick)[: n_y * slots_row].astype(BF16)

    with scope("e_pool_wait"):
        keep.wait()
        for d in range(1, n_tp):
            pool_copy(d).wait()

    def weight_copies(e):
        col, place = home(core * local_experts + e)
        pairs = [
            (w_gate.at[e], wgu.at[place, :, pl.ds(0, ff)]),
            (w_up.at[e], wgu.at[place, :, pl.ds(ff, ff)]),
            (w_down.at[e], wd.at[pl.ds(place * ff, ff)]),
        ]
        far = lambda: [remote(s, t, w_s.at[e, i], w_r.at[i, place], tp=col) for i, (s, t) in enumerate(pairs)]
        local = lambda: [pltpu.make_async_copy(s, t, w_r.at[i, place]) for i, (s, t) in enumerate(pairs)]
        return col, far, local

    with scope("c_wsend"):
        for e in range(local_experts):
            col, far, local = weight_copies(e)

            @pl.when(col != tp)
            def _():
                for copy in far():
                    copy.start()

            @pl.when(col == tp)
            def _():
                for copy in local():
                    copy.start()

    with scope("e_pool"):
        loads[1].wait()
        per = GROUP_DIM // channels
        for g in range(GROUPS):
            mixed_g = jnp.concatenate([tokmix[g * per + i] for i in range(per)], axis=1)
            cols = slice(g * GROUP_DIM, (g + 1) * GROUP_DIM)
            pooled[:, cols] = (dot(mixed_g, pool_wv[g]) * pool_s[:, cols]).astype(BF16)
        loads[2].wait()

        @pl.loop(0, width // tile)
        def _(n):
            wide[:, columns(n)] = dot(pooled[...], out_wv[:, columns(n)])

    def scaled(values, gain):
        inverse = lax.rsqrt(jnp.mean(values * values, axis=-1, keepdims=True) + norm_eps)
        return values * inverse * gain[...]

    with scope("e_norm"):
        loads[3].wait()

        @pl.loop(0, tok // part)
        def _(r):
            at = pl.ds(pl.multiple_of(r * part, part), part)
            residual = (resbuf[at, :].astype(F32) + scaled(wide[at, :], mix_g)).astype(BF16)
            resbuf[at, :] = residual
            normbuf[at, :] = scaled(residual.astype(F32), ffn_g).astype(BF16)

    with scope("f_disp"):
        @pl.loop(0, width // tile)
        def _(n):
            sent = dot(pick_rows, normbuf[:, columns(n)])
            disp[:, :, :, columns(n)] = sent.reshape(n_y, blocks, 8, tile).astype(BF16)

    by_distance = [d for i in range(1, n_y // 2) for d in (i, n_y - i)] + [n_y // 2]

    def y_copy(d):
        to = (y + d) % n_y
        return remote(disp.at[to], yarr.at[y], y_s.at[d], y_r.at[d], sp=at_y(to))

    y_keep = pltpu.make_async_copy(disp.at[y], yarr.at[y], y_r.at[0])
    y_keep.start()
    for d in by_distance:
        y_copy(d).start()

    order = [mine] + [(mine + i + row_experts) % row_experts for i in (sign, -sign)]
    order = order + [(mine + i) % row_experts for i in range(2, row_experts - 1)]

    def x_copy(k, row, main):
        j = order[k]
        col, place = home(j)
        if main:
            src, at = yarr.at[row, j], row
        else:
            src, at = ovout.at[j], n_y
        dst, sem = rows.at[0, place, at], x_r.at[place, at]
        if k == 0:
            return pltpu.make_async_copy(src, dst, sem)
        return remote(src, dst, x_s.at[k, at], sem, tp=col)

    with scope("f_relay"):
        for d in [0] + by_distance:
            if d == 0:
                y_keep.wait()
            else:
                y_copy(d).wait()
            row = (y - d + n_y) % n_y
            for k in range(row_experts):
                x_copy(k, row, True).start()

    with scope("g_regroup"):
        count = n_y * 8
        to_row = lax.broadcasted_iota(jnp.int32, (row_experts * n_y, count), 0)
        from_row = lax.broadcasted_iota(jnp.int32, (row_experts * n_y, count), 1)
        regroup = (from_row == to_row % n_y * 8 + to_row // n_y).astype(F32).astype(BF16)

        @pl.loop(0, width // tile)
        def _(n):
            moved = dot(regroup, rows_of(yarr[:, row_experts, :, columns(n)]))
            ovout[:, :, columns(n)] = moved.reshape(row_experts, n_y, tile).astype(BF16)

        for k in range(row_experts):
            x_copy(k, n_y, False).start()

    owner = mine // local_experts == core

    def forward_copies(d):
        shard = pl.ds(d * ff, ff)
        return [
            remote(wgu.at[d], wgu.at[d], f_s.at[0, d], f_r.at[0, d], sp=mate),
            remote(wd.at[shard], wd.at[shard], f_s.at[1, d], f_r.at[1, d], sp=mate),
        ]

    with scope("i_weights"):
        @pl.when(owner)
        def _():
            for d in range(near):
                landed(wgu.at[d, :, pl.ds(0, ff)], w_r.at[0, d])
                landed(wgu.at[d, :, pl.ds(ff, ff)], w_r.at[1, d])
                landed(wd.at[pl.ds(d * ff, ff)], w_r.at[2, d])
                for copy in forward_copies(d):
                    copy.start()

    def across(d):
        return remote(rows.at[0, d], rows.at[1, d], n_s.at[d], n_r.at[d], tp=other)

    with scope("i_across"):
        for d in range(near):
            for at in range(held):
                landed(rows.at[0, d, at], x_r.at[d, at])
            across(d).start()

    with scope("i_wmate"):
        @pl.when(jnp.logical_not(owner))
        def _():
            for d in range(near):
                landed(wgu.at[d], f_r.at[0, d])
                landed(wd.at[pl.ds(d * ff, ff)], f_r.at[1, d])

    def partial(d):
        return remote(given.at[d], taken.at[d], p_s.at[d], p_r.at[d], tp=other)

    def out_copy(d):
        return remote(orow.at[d], ret.at[mine], o_s.at[d], o_r.at[mine], tp=source(d))

    pair = 2
    some = 8 * held

    def evaluate(entered, q):
        for i in range(pair):
            d = q * pair + i
            if not entered:
                across(d).wait_recv()
            xb[i * some : (i + 1) * some, :] = rows_of(rows[0 if entered else 1, d])

        @pl.loop(0, near)
        def _(s):
            both = dot(xb[...], wgu[s])
            gate = jnp.minimum(both[:, :ff], clamp_limit)
            linear = jnp.clip(both[:, ff:], -clamp_limit, clamp_limit)
            cols = pl.ds(pl.multiple_of(s * ff, ff), ff)
            act[:, cols] = (gate * jax.nn.sigmoid(glu_alpha * gate) * (linear + 1.0)).astype(BF16)

        @pl.loop(0, width // tile)
        def _(n):
            result = dot(act[...], wd[:, columns(n)])
            for i in range(pair):
                piece = result[i * some : (i + 1) * some]
                if entered:
                    kept[q * pair + i, :, columns(n)] = piece
                else:
                    given[q * pair + i, :, :, columns(n)] = piece.reshape(held, 8, tile).astype(BF16)

        if not entered:
            for i in range(pair):
                partial(q * pair + i).start()

    def finish(q):
        for i in range(pair):
            d = q * pair + i
            partial(d).wait_recv()

            @pl.loop(0, width // tile)
            def _(n):
                both = kept[d, :, columns(n)].reshape(held, 8, tile) + taken[d, :, :, columns(n)].astype(F32)
                orow[d, :, :, columns(n)] = both.astype(BF16)

            if d == 0:
                pltpu.make_async_copy(orow.at[d], ret.at[mine], o_r.at[mine]).start()
            else:
                out_copy(d).start()

    for q in range(near // pair):
        with scope(f"j_near{q}"):
            evaluate(True, q)
        with scope(f"j_far{q}"):
            evaluate(False, q)
        if q:
            with scope(f"j_fin{q - 1}"):
                finish(q - 1)
    with scope("j_fin_last"):
        finish(near // pair - 1)

    def b_copy(k, d):
        to = (y + d) % n_y
        j = order[k]
        src, dst, sem = ret.at[j, to], fin.at[y, j], b_r.at[k, d]
        if d == 0:
            return pltpu.make_async_copy(src, dst, sem)
        return remote(src, dst, b_s.at[k, d], sem, sp=at_y(to))

    def v_copy(d):
        to = (y + d) % n_y
        src, dst, sem = ovback.at[to], fin.at[y, row_experts], v_r.at[d]
        if d == 0:
            return pltpu.make_async_copy(src, dst, sem)
        return remote(src, dst, v_s.at[d], sem, sp=at_y(to))

    with scope("k_back"):
        for k in range(row_experts):
            landed(ret.at[order[k]], o_r.at[order[k]])
            for d in by_distance + [0]:
                b_copy(k, d).start()

    with scope("l_back"):
        to_row = lax.broadcasted_iota(jnp.int32, (count, row_experts * n_y), 0)
        from_row = lax.broadcasted_iota(jnp.int32, (count, row_experts * n_y), 1)
        regroup_back = (from_row == to_row % 8 * n_y + to_row // 8).astype(F32)
        regroup_back = jnp.where(to_row % 8 < row_experts, regroup_back, 0.0).astype(BF16)

        @pl.loop(0, width // tile)
        def _(n):
            moved = dot(regroup_back, rows_of(ret[:, n_y, :, columns(n)]))
            ovback[:, :, columns(n)] = moved.reshape(n_y, 8, tile).astype(BF16)

        for d in by_distance + [0]:
            v_copy(d).start()

    with scope("m_finwait"):
        for d in [0] + by_distance:
            for k in range(row_experts):
                b_copy(k, d).wait()
            v_copy(d).wait()

    with scope("n_comb"):
        @pl.loop(0, width // tile)
        def _(n):
            came = rows_of(fin[:, :, :, columns(n)])
            came = jnp.concatenate([came, jnp.zeros((lanes - n_y * slots_row, tile), BF16)], axis=0)
            wide[:, columns(n)] = dot(whi[...], came) + dot(wlo[...], came)

        @pl.loop(0, tok // part)
        def _(r):
            at = pl.ds(pl.multiple_of(r * part, part), part)
            outbuf[at, :] = (resbuf[at, :].astype(F32) + scaled(wide[at, :], post_g)).astype(BF16)

        result = pltpu.make_async_copy(outbuf, out, lsem.at[0])
        result.start()

    with scope("o_drain"):
        for e in range(local_experts):
            col, far, local = weight_copies(e)

            @pl.when(col != tp)
            def _():
                for copy in far():
                    copy.wait_send()

        for k in range(1, row_experts):
            for row in range(n_y):
                x_copy(k, row, True).wait_send()
            x_copy(k, n_y, False).wait_send()

        @pl.when(owner)
        def _():
            for d in range(near):
                for copy in forward_copies(d):
                    copy.wait_send()

        for d in range(near):
            across(d).wait_send()
            partial(d).wait_send()
            if d:
                out_copy(d).wait_send()
        result.wait()


def per_device(
    resid_in, pool_input, pool_weight, pool_scale, out_weight, mix_gain, ffn_gain,
    w_gate, w_up, w_down, routes, route_weight, post_gain,
):
    n_sp = lax.axis_size("sp")
    n_tp = lax.axis_size("tp")
    n_y = n_sp // CORES
    seg, channels = pool_input.shape
    tok, width = resid_in.shape
    local_experts, _, ff = w_gate.shape
    row_experts = local_experts * CORES
    blocks = row_experts + 1
    slots = n_y * blocks * 8
    lanes = -(-slots // 128) * 128
    held = n_y + 1
    near = row_experts
    dma = pltpu.SemaphoreType.DMA
    vmem = pltpu.VMEM
    whole = pl.BlockSpec(memory_space=pltpu.VMEM)
    there = pl.BlockSpec(memory_space=pl.ANY)
    scratch = [
        vmem((halo_rows + seg, channels), BF16),
        vmem((seg, channels), BF16),
        vmem((n_tp, tok, channels), BF16),
        vmem(pool_weight.shape, BF16),
        vmem(out_weight.shape, BF16),
        vmem((tok, pool_scale.shape[0]), BF16),
        vmem((tok, width), F32),
        vmem((tok, width), BF16),
        vmem((tok, width), BF16),
        vmem((tok, lanes), BF16),
        vmem((tok, lanes), BF16),
        vmem((n_y, blocks, 8, width), BF16),
        vmem((n_y, blocks, 8, width), BF16),
        vmem((row_experts, 8, width), BF16),
        vmem((near, width, 2 * ff), BF16),
        vmem((near * ff, width), BF16),
        vmem((2, near, held, 8, width), BF16),
        vmem((2 * held * 8, width), BF16),
        vmem((2 * held * 8, near * ff), BF16),
        vmem((near, held * 8, width), F32),
        vmem((near, held, 8, width), BF16),
        vmem((near, held, 8, width), BF16),
        vmem((near, held, 8, width), BF16),
        vmem((row_experts, held, 8, width), BF16),
        vmem((n_y, 8, width), BF16),
        vmem((n_y, blocks, 8, width), BF16),
        vmem((tok, width), BF16),
        dma((4,)), dma, dma, dma((n_tp,)), dma((n_tp,)),
        dma((local_experts, 3)), dma((3, near)), dma((2, near)), dma((2, near)),
        dma((n_y,)), dma((n_y,)), dma((row_experts, held)), dma((near, held)),
        dma((near,)), dma((near,)), dma((near,)), dma((near,)),
        dma((near,)), dma((row_experts,)), dma((row_experts, n_y)), dma((row_experts, n_y)), dma((n_y,)), dma((n_y,)),
    ]
    return pl.pallas_call(
        functools.partial(kernel, n_sp, n_tp),
        out_shape=jax.ShapeDtypeStruct((tok, width), BF16),
        in_specs=[there, there, there, whole, there, whole, whole, there, there, there, whole, whole, whole],
        out_specs=there,
        scratch_shapes=scratch,
        compiler_params=pltpu.CompilerParams(
            collective_id=0, has_side_effects=True, vmem_limit_bytes=60 * 1024 * 1024
        ),
    )(
        pool_input, resid_in, pool_weight, pool_scale[None], out_weight, mix_gain[None], ffn_gain[None],
        w_gate, w_up, w_down, routes, route_weight, post_gain[None],
    )


def solution(mesh):
    in_specs = (
        P(("grp", "sp", "tp"), None),
        P(("grp", "sp"), "tp"),
        P(),
        P(),
        P(),
        P(),
        P(),
        P("sp", None, "tp"),
        P("sp", None, "tp"),
        P("sp", "tp", None),
        P(("grp", "sp", "tp"), None),
        P(("grp", "sp", "tp"), None),
        P(),
    )
    out_specs = P(("grp", "sp", "tp"), None)
    return jax.shard_map(
        per_device, mesh=mesh, in_specs=in_specs, out_specs=out_specs, check_vma=False
    )
```

```python
import functools

import jax
import jax.numpy as jnp
from jax import lax
from jax.experimental import pallas as pl
from jax.experimental.pallas import tpu as pltpu
from jax.sharding import PartitionSpec as P

GROUPS = 4
GROUP_DIM = 256
TOP = 2
CAP = 9
MAIN = 8
CORES = 2

pool_windows = (2, 4, 8, 16)
halo_rows = 16
norm_eps = 1e-06
clamp_limit = 7.0
glu_alpha = 1.702
MESH = pl.DeviceIdType.MESH
F32 = jnp.float32
BF16 = jnp.bfloat16


def dot(a, b):
    return jnp.dot(a, b, preferred_element_type=F32)


def rows_of(block):
    wide = block.astype(F32)
    return wide.reshape(-1, wide.shape[-1]).astype(BF16)


def kernel(
    n_sp, n_tp,
    pin, resid, pool_w, pool_s, out_w, mix_g, ffn_g, w_gate, w_up, w_down, routes, route_w, post_g,
    out,
    ext, mixbuf, tokmix, pool_wv, out_wv, pooled, wide, resbuf, normbuf, whi, wlo,
    disp, yarr, ovout, wgu, wd, rows, xb, act, orow, ret, ovback, fin, outbuf,
    lsem, halo_s, halo_r, pool_sem_s, pool_sem_r, w_s, w_r, f_s, f_r,
    z_s, z_r, q_s, q_r, y_s, y_r, x_s, x_r, o_s, o_r, b_s, b_r, v_s, v_r,
):
    n_y = n_sp // CORES
    local_experts = w_gate.shape[0]
    row_experts = local_experts * CORES
    step = n_tp // row_experts
    near = n_tp // step
    blocks = row_experts + 1
    slots_row = blocks * 8
    held = n_y + 1
    seg, channels = pin.shape
    tok, width = resid.shape
    ff = w_gate.shape[2]
    tile = 256
    part = 32
    scope = jax.named_scope
    sp = lax.axis_index("sp")
    tp = lax.axis_index("tp")
    y = sp // CORES
    core = sp % CORES
    mine = tp // step
    mate = y * CORES + (1 - core)
    grp = lax.axis_index("grp")
    half = grp % 2
    twin = grp + 1 - 2 * half
    side = tp % step
    sign = 2 * side - 1
    other = tp - sign

    def home(j):
        turn = (tp - step * j + 2 * n_tp - 1) % n_tp
        left = turn // near
        place = left * (near - 1 - turn % near) + (1 - left) * (turn % near)
        return step * j + 1 - left, place

    def source(d):
        return (tp + sign * d + n_tp) % n_tp

    def at_y(row):
        return row * CORES + core

    def remote(src, dst, send, recv, **where):
        return pltpu.make_async_remote_copy(
            src_ref=src, dst_ref=dst, send_sem=send, recv_sem=recv, device_id=where, device_id_type=MESH
        )

    def landed(dst, sem):
        pltpu.make_async_copy(dst, dst, sem).wait()

    def columns(n):
        return pl.ds(pl.multiple_of(n * tile, tile), tile)

    loads = [
        pltpu.make_async_copy(pin, ext.at[pl.ds(halo_rows, seg)], lsem.at[0]),
        pltpu.make_async_copy(pool_w, pool_wv, lsem.at[1]),
        pltpu.make_async_copy(out_w, out_wv, lsem.at[2]),
        pltpu.make_async_copy(resid, resbuf, lsem.at[3]),
    ]
    for load in loads:
        load.start()

    with scope("a_barrier"):
        barrier = pltpu.get_barrier_semaphore()
        for d in range(1, n_tp):
            pl.semaphore_signal(barrier, inc=1, device_id={"tp": (tp + d) % n_tp}, device_id_type=MESH)
        for d in range(1, n_y):
            pl.semaphore_signal(barrier, inc=1, device_id={"sp": at_y((y + d) % n_y)}, device_id_type=MESH)
        beside = (sp + 2 * core - 1 + n_sp) % n_sp
        pl.semaphore_signal(barrier, inc=1, device_id={"sp": mate}, device_id_type=MESH)
        pl.semaphore_signal(barrier, inc=1, device_id={"sp": beside}, device_id_type=MESH)
        pl.semaphore_signal(barrier, inc=1, device_id={"grp": twin}, device_id_type=MESH)
        pl.semaphore_wait(barrier, n_tp + n_y + 1)

    with scope("b_mix"):
        halo = remote(
            pin.at[pl.ds(seg - halo_rows, halo_rows)], ext.at[pl.ds(0, halo_rows)], halo_s, halo_r, sp=(sp + 1) % n_sp
        )
        halo.start()
        loads[0].wait()
        halo.wait()
        at = lax.broadcasted_iota(jnp.int32, (halo_rows + seg, 1), 0)
        own = ext[...].astype(F32)
        own = jnp.where(jnp.logical_and(at < halo_rows, sp == 0), 0.0, own)
        group = tp * channels // GROUP_DIM
        total, picked = own, own
        for level, window in enumerate(pool_windows):
            total = total + pltpu.roll(total, window // 2, 0)
            picked = jnp.where(group == level, total, picked)
        window = lax.shift_left(jnp.int32(2), group.astype(jnp.int32))
        divisor = jnp.minimum(sp * seg + at - halo_rows + 1, window).astype(F32)
        mixed = picked / jnp.maximum(divisor, 1.0) - own
        mixbuf[...] = mixed[halo_rows:].astype(BF16)

    def pool_copy(d):
        to = (tp + d) % n_tp
        return remote(
            mixbuf.at[pl.ds(to * tok, tok)], tokmix.at[tp], pool_sem_s.at[d], pool_sem_r.at[d], tp=to
        )

    keep = pltpu.make_async_copy(mixbuf.at[pl.ds(tp * tok, tok)], tokmix.at[tp], pool_sem_r.at[0])
    keep.start()
    for d in range(1, n_tp):
        pool_copy(d).start()

    with scope("d_route"):
        lanes = whi.shape[1]
        expert_lane = lax.broadcasted_iota(jnp.int32, (tok, 128), 1)
        before = (
            lax.broadcasted_iota(jnp.int32, (tok, tok), 1) < lax.broadcasted_iota(jnp.int32, (tok, tok), 0)
        ).astype(F32).astype(BF16)
        named = [routes[:, k : k + 1] for k in range(TOP)]
        onehot = [(named[k] == expert_lane).astype(F32) for k in range(TOP)]
        earlier = jnp.zeros((1, 128), F32)
        slot_lane = lax.broadcasted_iota(jnp.int32, (1, lanes), 1)
        inside = slot_lane % slots_row
        spill = inside >= row_experts * MAIN
        row_expert = jnp.where(spill, inside - row_experts * MAIN, inside // MAIN)
        slot_rank = jnp.where(spill, MAIN, inside % MAIN).astype(F32)
        valid = jnp.logical_and(row_expert < row_experts, slot_lane < n_y * slots_row)
        slot_expert = jnp.where(valid, slot_lane // slots_row * row_experts + row_expert, -1)
        pick = jnp.zeros((tok, lanes), F32)
        comb = jnp.zeros((tok, lanes), F32)
        for k in range(TOP):
            ranks = dot(before, onehot[k].astype(BF16)) + earlier
            rank = jnp.sum(ranks * onehot[k], axis=1, keepdims=True)
            earlier = earlier + jnp.sum(onehot[k], axis=0, keepdims=True)
            hit = jnp.logical_and(named[k] == slot_expert, rank == slot_rank).astype(F32)
            pick = pick + hit
            comb = comb + hit * route_w[:, k : k + 1]
        high = comb.astype(BF16)
        whi[...] = high
        wlo[...] = (comb - high.astype(F32)).astype(BF16)
        pick_rows = jnp.transpose(pick)[: n_y * slots_row].astype(BF16)

    with scope("e_pool_wait"):
        keep.wait()
        for d in range(1, n_tp):
            pool_copy(d).wait()

    owner = mine // local_experts == core
    items = 3
    deep = width // 4
    short = ff // 2

    def item(slot, which, i):
        if i == items - 1:
            return wd.at[pl.ds(slot * ff + which * short, short)]
        return wgu.at[slot, pl.ds(which * 2 * deep + i * deep, deep)]

    def both_whole(slot):
        return wgu.at[slot], wd.at[pl.ds(slot * ff, ff)]

    def weight_copies(e, i):
        col, place = home(core * local_experts + e)
        slot = col % step * near + place
        if i == items - 1:
            pairs = [(w_down.at[e, pl.ds(half * short, short)], item(slot, half, i))]
        else:
            at = pl.ds(half * 2 * deep + i * deep, deep)
            pairs = [
                (w_gate.at[e, at], wgu.at[slot, at, pl.ds(0, ff)]),
                (w_up.at[e, at], wgu.at[slot, at, pl.ds(ff, ff)]),
            ]
        far = lambda: [remote(s, t, w_s.at[e, i, n], w_r.at[i, place], tp=col) for n, (s, t) in enumerate(pairs)]
        return col, far

    def own_shard():
        slot = side * near
        e = mine % local_experts
        pairs = [
            (w_gate.at[e], wgu.at[slot, :, pl.ds(0, ff)]),
            (w_up.at[e], wgu.at[slot, :, pl.ds(ff, ff)]),
            (w_down.at[e], wd.at[pl.ds(slot * ff, ff)]),
        ]
        local = lambda: [pltpu.make_async_copy(s, t, w_r.at[n, 0]) for n, (s, t) in enumerate(pairs)]
        over = lambda: [remote(s, t, q_s.at[n, 0], q_r.at[n, 0], tp=other) for n, (s, t) in enumerate(pairs)]
        return local, over

    with scope("c_wsend"):
        @pl.when(owner)
        def _():
            local, over = own_shard()
            for copy in local() + over():
                copy.start()

        for i in range(items):
            for e in range(local_experts):
                col, far = weight_copies(e, i)

                @pl.when(col != tp)
                def _():
                    for copy in far():
                        copy.start()

    def swap_copy(at_side, d, i):
        src = item(at_side * near + d, half, i)
        rel = (at_side - side) * (at_side - side)
        return remote(src, src, z_s.at[rel, d, i], z_r.at[rel, d, i], grp=twin)

    def over_copy(d, i):
        src = item(side * near + d, half, i)
        return remote(src, src, q_s.at[i, d], q_r.at[i, d], tp=other)

    def mate_copy(at_side, d, which, i):
        slot = at_side * near + d
        rel = (at_side - side) * (at_side - side)
        src = item(slot, half if which == 0 else 1 - half, i) if d else both_whole(slot)[i]
        return remote(src, src, f_s.at[rel, d, which, i], f_r.at[rel, d, which, i], sp=mate)

    def own_came():
        @pl.when(owner)
        def _():
            slot = side * near
            landed(wgu.at[slot, :, pl.ds(0, ff)], w_r.at[0, 0])
            landed(wgu.at[slot, :, pl.ds(ff, ff)], w_r.at[1, 0])
            landed(wd.at[pl.ds(slot * ff, ff)], w_r.at[2, 0])
            for i in range(2):
                mate_copy(side, 0, 0, i).start()

    def over_own_came():
        @pl.when(owner)
        def _():
            slot = (1 - side) * near
            landed(wgu.at[slot, :, pl.ds(0, ff)], q_r.at[0, 0])
            landed(wgu.at[slot, :, pl.ds(ff, ff)], q_r.at[1, 0])
            landed(wd.at[pl.ds(slot * ff, ff)], q_r.at[2, 0])
            for i in range(2):
                mate_copy(1 - side, 0, 0, i).start()

    def came(i):
        @pl.when(owner)
        def _():
            for d in range(1, near):
                landed(item(side * near + d, half, i), w_r.at[i, d])
                over_copy(d, i).start()
                swap_copy(side, d, i).start()
                mate_copy(side, d, 0, i).start()

    def over_came(i):
        @pl.when(owner)
        def _():
            for d in range(1, near):
                landed(item((1 - side) * near + d, half, i), q_r.at[i, d])
                swap_copy(1 - side, d, i).start()
                mate_copy(1 - side, d, 0, i).start()

    def swap_came(i):
        @pl.when(owner)
        def _():
            for rel in range(2):
                at_side = side + rel - 2 * rel * side
                for d in range(1, near):
                    landed(item(at_side * near + d, 1 - half, i), z_r.at[rel, d, i])
                    mate_copy(at_side, d, 1, i).start()

    with scope("e_pool"):
        loads[1].wait()
        per = GROUP_DIM // channels
        for g in range(GROUPS):
            mixed_g = jnp.concatenate([tokmix[g * per + i] for i in range(per)], axis=1)
            cols = slice(g * GROUP_DIM, (g + 1) * GROUP_DIM)
            pooled[:, cols] = (dot(mixed_g, pool_wv[g]) * pool_s[:, cols]).astype(BF16)
        loads[2].wait()

        @pl.loop(0, width // tile)
        def _(n):
            wide[:, columns(n)] = dot(pooled[...], out_wv[:, columns(n)])

    def scaled(values, gain):
        inverse = lax.rsqrt(jnp.mean(values * values, axis=-1, keepdims=True) + norm_eps)
        return values * inverse * gain[...]

    with scope("e_norm"):
        loads[3].wait()

        @pl.loop(0, tok // part)
        def _(r):
            at = pl.ds(pl.multiple_of(r * part, part), part)
            residual = (resbuf[at, :].astype(F32) + scaled(wide[at, :], mix_g)).astype(BF16)
            resbuf[at, :] = residual
            normbuf[at, :] = scaled(residual.astype(F32), ffn_g).astype(BF16)

    with scope("f_disp"):
        @pl.loop(0, width // tile)
        def _(n):
            sent = dot(pick_rows, normbuf[:, columns(n)])
            disp[:, :, :, columns(n)] = sent.reshape(n_y, blocks, 8, tile).astype(BF16)

    by_distance = [d for i in range(1, n_y // 2) for d in (i, n_y - i)] + [n_y // 2]

    def y_copy(d):
        to = (y + d) % n_y
        return remote(disp.at[to], yarr.at[y], y_s.at[d], y_r.at[d], sp=at_y(to))

    y_keep = pltpu.make_async_copy(disp.at[y], yarr.at[y], y_r.at[0])
    y_keep.start()
    for d in by_distance:
        y_copy(d).start()

    order = [mine] + [(mine + i + row_experts) % row_experts for i in (sign, -sign)]
    order = order + [(mine + i) % row_experts for i in range(2, row_experts - 1)]

    def x_copy(k, row, main):
        j = order[k]
        col, place = home(j)
        if main:
            src, at = yarr.at[row, j], row
        else:
            src, at = ovout.at[j], n_y
        dst, sem = rows.at[place, at], x_r.at[place, at]
        if k == 0:
            return pltpu.make_async_copy(src, dst, sem)
        return remote(src, dst, x_s.at[k, at], sem, tp=col)

    with scope("f_relay"):
        for d in [0] + by_distance:
            if d == 0:
                y_keep.wait()
            else:
                y_copy(d).wait()
            row = (y - d + n_y) % n_y
            for k in range(row_experts):
                x_copy(k, row, True).start()
            if d == 0:
                own_came()
            elif d == by_distance[1]:
                came(0)
            elif d == by_distance[3]:
                over_own_came()
                came(1)
                over_came(0)
            elif d == by_distance[5]:
                came(2)
                over_came(1)

    with scope("g_regroup"):
        count = n_y * 8
        to_row = lax.broadcasted_iota(jnp.int32, (row_experts * n_y, count), 0)
        from_row = lax.broadcasted_iota(jnp.int32, (row_experts * n_y, count), 1)
        regroup = (from_row == to_row % n_y * 8 + to_row // n_y).astype(F32).astype(BF16)

        @pl.loop(0, width // tile)
        def _(n):
            moved = dot(regroup, rows_of(yarr[:, row_experts, :, columns(n)]))
            ovout[:, :, columns(n)] = moved.reshape(row_experts, n_y, tile).astype(BF16)

        for k in range(row_experts):
            x_copy(k, n_y, False).start()

    with scope("i_weights"):
        over_came(2)
        for i in range(items):
            swap_came(i)

    with scope("i_wmate"):
        @pl.when(jnp.logical_not(owner))
        def _():
            for rel in range(2):
                at_side = side + rel - 2 * rel * side
                for i, piece in enumerate(both_whole(at_side * near)):
                    landed(piece, f_r.at[rel, 0, 0, i])
                for which in range(2):
                    for d in range(1, near):
                        for i in range(items):
                            piece = item(at_side * near + d, half if which == 0 else 1 - half, i)
                            landed(piece, f_r.at[rel, d, which, i])

    def out_copy(d):
        return remote(orow.at[d], ret.at[mine], o_s.at[d], o_r.at[mine], tp=source(d))

    pair = 2
    some = 8 * held

    def evaluate(q):
        for i in range(pair):
            d = q * pair + i
            for at in range(held):
                landed(rows.at[d, at], x_r.at[d, at])
            xb[i * some : (i + 1) * some, :] = rows_of(rows[d])

        @pl.loop(0, n_tp)
        def _(s):
            both = dot(xb[...], wgu[s])
            gate = jnp.minimum(both[:, :ff], clamp_limit)
            linear = jnp.clip(both[:, ff:], -clamp_limit, clamp_limit)
            cols = pl.ds(pl.multiple_of(s * ff, ff), ff)
            act[:, cols] = (gate * jax.nn.sigmoid(glu_alpha * gate) * (linear + 1.0)).astype(BF16)

        @pl.loop(0, width // tile)
        def _(n):
            result = dot(act[...], wd[:, columns(n)])
            for i in range(pair):
                piece = result[i * some : (i + 1) * some]
                orow[q * pair + i, :, :, columns(n)] = piece.reshape(held, 8, tile).astype(BF16)

        for i in range(pair):
            d = q * pair + i
            if d == 0:
                pltpu.make_async_copy(orow.at[d], ret.at[mine], o_r.at[mine]).start()
            else:
                out_copy(d).start()

    for q in range(near // pair):
        with scope(f"j_eval{q}"):
            evaluate(q)

    def back(k):
        landed(ret.at[order[k]], o_r.at[order[k]])
        for d in by_distance + [0]:
            b_copy(k, d).start()

    def b_copy(k, d):
        to = (y + d) % n_y
        j = order[k]
        src, dst, sem = ret.at[j, to], fin.at[y, j], b_r.at[k, d]
        if d == 0:
            return pltpu.make_async_copy(src, dst, sem)
        return remote(src, dst, b_s.at[k, d], sem, sp=at_y(to))

    def v_copy(d):
        to = (y + d) % n_y
        src, dst, sem = ovback.at[to], fin.at[y, row_experts], v_r.at[d]
        if d == 0:
            return pltpu.make_async_copy(src, dst, sem)
        return remote(src, dst, v_s.at[d], sem, sp=at_y(to))

    for q in range(near // pair):
        with scope(f"k_back{q}"):
            for k in range(q * pair, (q + 1) * pair):
                back(k)

    with scope("l_back"):
        to_row = lax.broadcasted_iota(jnp.int32, (count, row_experts * n_y), 0)
        from_row = lax.broadcasted_iota(jnp.int32, (count, row_experts * n_y), 1)
        regroup_back = (from_row == to_row % 8 * n_y + to_row // 8).astype(F32)
        regroup_back = jnp.where(to_row % 8 < row_experts, regroup_back, 0.0).astype(BF16)

        @pl.loop(0, width // tile)
        def _(n):
            moved = dot(regroup_back, rows_of(ret[:, n_y, :, columns(n)]))
            ovback[:, :, columns(n)] = moved.reshape(n_y, 8, tile).astype(BF16)

        for d in by_distance + [0]:
            v_copy(d).start()

    with scope("m_finwait"):
        for d in [0] + by_distance:
            for k in range(row_experts):
                b_copy(k, d).wait()
            v_copy(d).wait()

    with scope("n_comb"):
        @pl.loop(0, width // tile)
        def _(n):
            came = rows_of(fin[:, :, :, columns(n)])
            came = jnp.concatenate([came, jnp.zeros((lanes - n_y * slots_row, tile), BF16)], axis=0)
            wide[:, columns(n)] = dot(whi[...], came) + dot(wlo[...], came)

        @pl.loop(0, tok // part)
        def _(r):
            at = pl.ds(pl.multiple_of(r * part, part), part)
            outbuf[at, :] = (resbuf[at, :].astype(F32) + scaled(wide[at, :], post_g)).astype(BF16)

        result = pltpu.make_async_copy(outbuf, out, lsem.at[0])
        result.start()

    with scope("o_drain"):
        for i in range(items):
            for e in range(local_experts):
                col, far = weight_copies(e, i)

                @pl.when(col != tp)
                def _():
                    for copy in far():
                        copy.wait_send()

        for k in range(1, row_experts):
            for row in range(n_y):
                x_copy(k, row, True).wait_send()
            x_copy(k, n_y, False).wait_send()

        @pl.when(owner)
        def _():
            for copy in own_shard()[1]():
                copy.wait_send()
            for rel in range(2):
                at_side = side + rel - 2 * rel * side
                for i in range(2):
                    mate_copy(at_side, 0, 0, i).wait_send()
                for d in range(1, near):
                    for i in range(items):
                        if rel == 0:
                            over_copy(d, i).wait_send()
                        swap_copy(at_side, d, i).wait_send()
                        for which in range(2):
                            mate_copy(at_side, d, which, i).wait_send()

        for d in range(1, near):
            out_copy(d).wait_send()
        result.wait()


def per_device(
    resid_in, pool_input, pool_weight, pool_scale, out_weight, mix_gain, ffn_gain,
    w_gate, w_up, w_down, routes, route_weight, post_gain,
):
    n_sp = lax.axis_size("sp")
    n_tp = lax.axis_size("tp")
    n_y = n_sp // CORES
    seg, channels = pool_input.shape
    tok, width = resid_in.shape
    local_experts, _, ff = w_gate.shape
    row_experts = local_experts * CORES
    blocks = row_experts + 1
    slots = n_y * blocks * 8
    lanes = -(-slots // 128) * 128
    held = n_y + 1
    near = row_experts
    dma = pltpu.SemaphoreType.DMA
    vmem = pltpu.VMEM
    whole = pl.BlockSpec(memory_space=pltpu.VMEM)
    there = pl.BlockSpec(memory_space=pl.ANY)
    scratch = [
        vmem((halo_rows + seg, channels), BF16),
        vmem((seg, channels), BF16),
        vmem((n_tp, tok, channels), BF16),
        vmem(pool_weight.shape, BF16),
        vmem(out_weight.shape, BF16),
        vmem((tok, pool_scale.shape[0]), BF16),
        vmem((tok, width), F32),
        vmem((tok, width), BF16),
        vmem((tok, width), BF16),
        vmem((tok, lanes), BF16),
        vmem((tok, lanes), BF16),
        vmem((n_y, blocks, 8, width), BF16),
        vmem((n_y, blocks, 8, width), BF16),
        vmem((row_experts, 8, width), BF16),
        vmem((n_tp, width, 2 * ff), BF16),
        vmem((n_tp * ff, width), BF16),
        vmem((near, held, 8, width), BF16),
        vmem((2 * held * 8, width), BF16),
        vmem((2 * held * 8, n_tp * ff), BF16),
        vmem((near, held, 8, width), BF16),
        vmem((row_experts, held, 8, width), BF16),
        vmem((n_y, 8, width), BF16),
        vmem((n_y, blocks, 8, width), BF16),
        vmem((tok, width), BF16),
        dma((4,)), dma, dma, dma((n_tp,)), dma((n_tp,)),
        dma((local_experts, 3, 2)), dma((3, near)), dma((2, near, 2, 3)), dma((2, near, 2, 3)),
        dma((2, near, 3)), dma((2, near, 3)), dma((3, near)), dma((3, near)),
        dma((n_y,)), dma((n_y,)), dma((row_experts, held)), dma((near, held)),
        dma((near,)), dma((row_experts,)), dma((row_experts, n_y)), dma((row_experts, n_y)), dma((n_y,)), dma((n_y,)),
    ]
    return pl.pallas_call(
        functools.partial(kernel, n_sp, n_tp),
        out_shape=jax.ShapeDtypeStruct((tok, width), BF16),
        in_specs=[there, there, there, whole, there, whole, whole, there, there, there, whole, whole, whole],
        out_specs=there,
        scratch_shapes=scratch,
        compiler_params=pltpu.CompilerParams(
            collective_id=0, has_side_effects=True, vmem_limit_bytes=60 * 1024 * 1024
        ),
    )(
        pool_input, resid_in, pool_weight, pool_scale[None], out_weight, mix_gain[None], ffn_gain[None],
        w_gate, w_up, w_down, routes, route_weight, post_gain[None],
    )


def solution(mesh):
    in_specs = (
        P(("grp", "sp", "tp"), None),
        P(("grp", "sp"), "tp"),
        P(),
        P(),
        P(),
        P(),
        P(),
        P("sp", None, "tp"),
        P("sp", None, "tp"),
        P("sp", "tp", None),
        P(("grp", "sp", "tp"), None),
        P(("grp", "sp", "tp"), None),
        P(),
    )
    out_specs = P(("grp", "sp", "tp"), None)
    return jax.shard_map(
        per_device, mesh=mesh, in_specs=in_specs, out_specs=out_specs, check_vma=False
    )
```
